32 devices in a mesh: sp: 16 (over z, y, x), tp: 2 (over core).
Axes of the slice: x: 2, y: 2, z: 4, core: 2. Of those that a mesh axis runs over, the one named last changes fastest.
Arguments:
- queries: bfloat16 [2048, 1024], P('sp', 'tp'), may hold values from -6 to 6
- keys: bfloat16 [2048, 1024], P('sp', 'tp'), may hold values from -6 to 6
- values: bfloat16 [2048, 2048], P('sp', 'tp'), may hold values from -6 to 6
- out_gate: bfloat16 [2048, 2048], P('sp', 'tp'), may hold values from -6 to 6
- decay_rate: float32 [8], P('tp'), may hold values from 0 to 1
- residual: bfloat16 [2048, 2048], P(('sp', 'tp')), may hold values from -6 to 6
- out_weight: bfloat16 [2048, 2048], P('tp'), may hold values from -0.125 to 0.125
- ffn_gain: float32 [2048], replicated, may hold values from 0.1 to 1.9
- route_ids: int32 [2048, 4], P(('sp', 'tp')), may hold values from 0 to 15, all different within a row; in each aligned block of 64 rows (0 to 63, 64 to 127, ...) at most 32 rows name the same one
- route_weights: float32 [2048, 4], P(('sp', 'tp')), may hold values from 0.1 to 1
- gate_up: bfloat16 [16, 2048, 2048], P('sp', None, 'tp'), may hold values from -0.375 to 0.375
- lin_up: bfloat16 [16, 2048, 2048], P('sp', None, 'tp'), may hold values from -0.375 to 0.375
- down_weight: bfloat16 [16, 2048, 2048], P('sp', 'tp'), may hold values from -0.03125 to 0.03125
Outputs:
- layer_out: bfloat16 [2048, 2048], P(('sp', 'tp'))
The draws below stay inside these ranges and needn't reach their ends.
Inputs may be any that keep to these rules, and one draw needn't show every extreme that they name: `route_ids`: within the rows of one device (aligned blocks of 64 rows), no expert is named by more than 32 entries, a bound that some block reaches; the 4 experts of a row differ.
All inputs are finite; a program needn't handle non-finite values.
Results may differ from the reference program's by a relative error of at most 0.03.
Values may be sent and summed in bfloat16 or wider, within the bound.
A program may use at most 128 MiB of HBM per device.

```python
import math
import jax
import jax.numpy as jnp
import numpy as np
from jax import lax

D = 2048
HEADS = 8
DK = 128
DV = 256
DE = 2048
TOPK = 4
TOK_DEV = 128
EXPERTS = 16
TOKENS = 2048
ROWS = 64
CAP = 32
N_SP = 16
N_TP = 2


def draw_decay_rate(key, part):
    first_key, second_key = jax.random.split(key, 2)
    spread = jax.random.uniform(first_key, (HEADS,), jnp.float32)
    slow_low = jnp.log(0.2 / TOKENS)
    slow_high = jnp.log(2.0 / TOKENS)
    fast_low = jnp.log(1.0 / 100.0)
    fast_high = jnp.log(1.0 / 30.0)
    slow_rate = jnp.exp(slow_low + spread * (slow_high - slow_low))
    fast_rate = jnp.exp(fast_low + spread * (fast_high - fast_low))
    order = jax.random.permutation(second_key, HEADS)
    fast_count = HEADS // 2
    return jnp.where(order < fast_count, fast_rate, slow_rate).astype(jnp.float32)


def levels(stream_key, shape, shards, least, largest):
    factor_of, own = 1.0, jax.random.fold_in(stream_key, 6)
    for dim, shards_of in shards:
        steps = jnp.exp(jax.random.uniform(jax.random.fold_in(own, dim), (shards_of,), jnp.float32, least / len(shards), largest / len(shards)))
        factor_of = factor_of * jnp.repeat(steps, shape[dim] // shards_of).reshape([-1 if axis == dim else 1 for axis in range(len(shape))])
    return factor_of


def deal_out(key, own, number, rows, number_of, top, bound, lean):
    sequence = jax.random.permutation(key, number_of)
    heavy_load, usual = load_shares(number_of, rows * top, bound, lean, True), load_shares(number_of, rows * top, bound, lean, False)
    places = jnp.arange(number_of)

    def named(sizes, turn):
        used = int((sizes > 0).sum())
        fixed = max(1, used // 4)
        shifted = fixed + (places - fixed + turn * (used - fixed)) % max(1, number_of - fixed)
        return jnp.zeros((number_of,), jnp.int32).at[sequence[jnp.where(places < fixed, places, shifted)]].set(jnp.asarray(sizes, jnp.int32))

    sizes = jnp.where(number % 4 == 0, named(heavy_load, number // 4), named(usual, number - number // 4 - 1))
    mixed = jax.random.permutation(jax.random.fold_in(own, 3), number_of)
    source_of, sink = mixed[0:number_of // 2 * 2:2], mixed[1:number_of // 2 * 2:2]
    room = jnp.minimum(sizes[source_of] - 1, bound - sizes[sink]) // 2
    room = jnp.where((source_of == sequence[0]) | (sink == sequence[0]) | (sizes[sink] == 0), 0, jnp.maximum(room, 0))
    shifted = jax.random.randint(jax.random.fold_in(own, 4), (number_of // 2,), 0, 1 << 20) % (room + 1)
    sizes = sizes.at[source_of].add(-shifted).at[sink].add(shifted)
    items = jnp.searchsorted(jnp.cumsum(sizes), jnp.arange(rows * top), side="right").astype(jnp.int32)
    table = items.reshape(top, rows).T
    table = table[jax.random.permutation(jax.random.fold_in(own, 1), rows)]
    turn = jax.random.randint(jax.random.fold_in(own, 2), (rows, 1), 0, top)
    return jnp.take_along_axis(table, (jnp.arange(top)[None, :] + turn) % top, axis=1)


def load_shares(amount, total, limit, slope, full):
    loads = [(1 << 20) // math.isqrt(standing ** slope) + 1 for standing in range(1, amount + 1)]
    largest = limit if full else min(limit, max(-(-total // amount), total * loads[0] // sum(loads)))
    least = 1 if total - largest >= amount - 1 else 0
    given, surplus = [largest] + [least] * (amount - 1), total - largest - least * (amount - 1)
    while surplus > 0:
        free = [i for i in range(1, amount) if given[i] < largest] or [i for i in range(1, amount) if given[i] < limit]
        pool, left = sum([loads[i] for i in free]), surplus
        for i in free:
            extra = min(limit - given[i], max(1, left * loads[i] // pool), surplus)
            given[i] = given[i] + extra
            surplus = surplus - extra
    return np.array(given)


def gaussian(own_key, extent, scale, most, cuts=(), kind=jnp.bfloat16):
    drawn = jax.random.normal(own_key, extent, jnp.float32) * scale
    if len(cuts) > 0:
        drawn = levels(own_key, extent, cuts, -0.22, 0.18) * drawn
    return jnp.clip(drawn, min=-most, max=most).astype(kind)


def setup_inputs(seed: int = 0) -> dict:
    streams_of = jax.random.split(jax.random.key(seed), 14)
    queries = gaussian(streams_of[0], (TOKENS, HEADS * DK), 1.0, 6.0, ((0, 16), (1, 2)))
    keys = gaussian(streams_of[1], (TOKENS, HEADS * DK), 1.0, 6.0, ((0, 16), (1, 2)))
    values = gaussian(streams_of[2], (TOKENS, HEADS * DV), 1.0, 6.0, ((0, 16), (1, 2)))
    out_gate = gaussian(streams_of[3], (TOKENS, HEADS * DV), 1.0, 6.0, ((0, 16), (1, 2)))
    decay_rate = draw_decay_rate(jax.random.fold_in(streams_of[13], 71), 0)
    residual = gaussian(streams_of[5], (TOKENS, D), 1.0, 6.0, ((0, 32),))
    out_weight = gaussian(streams_of[6], (HEADS * DV, D), (HEADS * DV) ** -0.5, 0.125, ((0, 2),))
    ffn_gain = jnp.clip(1.0 + 0.18 * jax.random.normal(streams_of[7], (D,), jnp.float32), 0.1, 1.9)
    route_ids_keys = jax.random.split(jax.random.fold_in(streams_of[8], 1), TOKENS // ROWS)
    route_ids_turns = jax.random.permutation(jax.random.fold_in(streams_of[8], 3), TOKENS // ROWS)
    route_ids = jax.vmap(lambda own, number: deal_out(jax.random.fold_in(streams_of[8], 2), own, number, ROWS, EXPERTS, TOPK, CAP, 1))(route_ids_keys, route_ids_turns).reshape((TOKENS, TOPK))
    route_weights = jnp.clip(jnp.exp(math.log(1.0) - 2.3025851 * jax.random.uniform(streams_of[9], (TOKENS, TOPK), jnp.float32) ** levels(streams_of[9], (TOKENS, TOPK), ((0, 32),), -0.2, 0.2)), 0.1, 1.0)
    gate_up = gaussian(streams_of[10], (EXPERTS, D, DE), (D // 9) ** -0.5, 0.375, ((0, 16), (2, 2)))
    lin_up = gaussian(streams_of[11], (EXPERTS, D, DE), (D // 9) ** -0.5, 0.375, ((0, 16), (2, 2)))
    down_weight = gaussian(streams_of[12], (EXPERTS, DE, D), (DE * 16) ** -0.5, 0.03125, ((0, 16), (1, 2)))
    return dict(queries=queries, keys=keys, values=values, out_gate=out_gate, decay_rate=decay_rate, residual=residual, out_weight=out_weight, ffn_gain=ffn_gain, route_ids=route_ids, route_weights=route_weights, gate_up=gate_up, lin_up=lin_up, down_weight=down_weight)


EPS = 1e-05
CLAMP_LIMIT = 7.0
SIGMOID_SLOPE = 1.702
TOP_PRECISION = lax.Precision.HIGHEST

def expert_act(row_block, gate_part, lin_part):
    gate_pre = jnp.dot(row_block, gate_part, preferred_element_type=jnp.float32)
    lin_pre = jnp.dot(row_block, lin_part, preferred_element_type=jnp.float32)
    gate_clip = jnp.minimum(gate_pre, CLAMP_LIMIT)
    lin_clip = jnp.clip(lin_pre, -CLAMP_LIMIT, CLAMP_LIMIT)
    return (gate_clip * jax.nn.sigmoid(SIGMOID_SLOPE * gate_clip) * (lin_clip + 1.0)).astype(jnp.bfloat16)

def reference(queries, keys, values, out_gate, decay_rate, residual, out_weight, ffn_gain, route_ids, route_weights, gate_up, lin_up, down_weight):
    total_tokens = queries.shape[0]
    block_len = TOK_DEV
    block_count = total_tokens // block_len
    log_gamma = -decay_rate.astype(jnp.float32)
    query_heads = queries.astype(jnp.float32).reshape(block_count, block_len, HEADS, DK).transpose(0, 2, 1, 3)
    per_head_keys = keys.astype(jnp.float32).reshape(block_count, block_len, HEADS, DK).transpose(0, 2, 1, 3) * DK ** (-0.5)
    per_head_values = values.astype(jnp.float32).reshape(block_count, block_len, HEADS, DV).transpose(0, 2, 1, 3)
    positions = jnp.arange(block_len, dtype=jnp.float32)
    offsets = positions[:, None] - positions[None, :]
    causal = offsets >= 0
    decay_mask = jnp.where(causal[None], jnp.exp(jnp.where(causal, offsets, 0.0)[None] * log_gamma[:, None, None]), 0.0)
    trailing_decay = jnp.exp((block_len - 1.0 - positions)[None, :] * log_gamma[:, None])
    lead_decay = jnp.exp((positions + 1.0)[None, :] * log_gamma[:, None])
    chain_decay = jnp.exp(block_len * log_gamma)

    def block_step(carried, block):
        query_block, block_keys, block_values = block
        attention_scores = jnp.einsum('hqd,hkd->hqk', query_block, block_keys, precision=TOP_PRECISION) * decay_mask
        intra_block_term = jnp.einsum('zfp,zpn->zfn', attention_scores, block_values, precision=TOP_PRECISION)
        cross_term = jnp.einsum('hqd,hdv->hqv', query_block, carried, precision=TOP_PRECISION) * lead_decay[:, :, None]
        state_delta = jnp.einsum('mxs,mxq->msq', block_keys * trailing_decay[:, :, None], block_values, precision=TOP_PRECISION)
        new_state = chain_decay[:, None, None] * carried + state_delta
        return (new_state, intra_block_term + cross_term)
    _, outputs = lax.scan(block_step, jnp.zeros((HEADS, DK, DV), jnp.float32), (query_heads, per_head_keys, per_head_values))
    retained = outputs.transpose(0, 2, 1, 3).reshape(total_tokens, HEADS, DV)
    normed = retained * lax.rsqrt(lax.optimization_barrier(jnp.mean(retained * retained, axis=-1, keepdims=True)) + EPS)
    gated = (normed.reshape(total_tokens, HEADS * DV) * jax.nn.silu(out_gate.astype(jnp.float32))).astype(jnp.bfloat16)
    group_width = HEADS * DV // N_TP
    mix_rows = jnp.zeros((total_tokens, D), jnp.float32)
    for group in range(N_TP):
        partial_value = jnp.dot(gated[:, group * group_width:(group + 1) * group_width], out_weight[group * group_width:(group + 1) * group_width], preferred_element_type=jnp.float32).astype(jnp.bfloat16)
        mix_rows = mix_rows + lax.optimization_barrier(partial_value).astype(jnp.float32)
    mixed = (residual.astype(jnp.float32) + mix_rows).astype(jnp.bfloat16)
    mixed_wide = mixed.astype(jnp.float32)
    normed_rows = (mixed_wide * lax.rsqrt(lax.optimization_barrier(jnp.mean(mixed_wide * mixed_wide, axis=-1, keepdims=True)) + EPS) * ffn_gain.astype(jnp.float32)).astype(jnp.bfloat16)
    device_count = N_SP * N_TP
    own_rows = total_tokens // device_count
    block_ids = route_ids.reshape(device_count, own_rows * TOPK).astype(jnp.int32)
    one_hot = (block_ids[:, :, None] == jnp.arange(EXPERTS, dtype=jnp.int32)[None, None, :]).astype(jnp.int32)
    slot_rank = lax.optimization_barrier(jnp.sum(one_hot * (jnp.cumsum(one_hot, axis=1) - 1), axis=2))
    device_index = jnp.arange(device_count, dtype=jnp.int32)[:, None]
    slot_index = (block_ids * (device_count * CAP) + device_index * CAP + slot_rank).reshape(-1).astype(jnp.int32)
    source_row = (jnp.arange(total_tokens * TOPK, dtype=jnp.int32) // TOPK).astype(jnp.int32)
    slot_source = jnp.full((EXPERTS * device_count * CAP,), total_tokens, jnp.int32).at[slot_index].set(source_row)
    padded = jnp.concatenate([normed_rows, jnp.zeros((1, D), jnp.bfloat16)], axis=0)
    half_width = DE // N_TP

    def run_expert(packed):
        sources, gate_full, lin_full, down_full = packed
        activation = expert_act(padded[sources], gate_full, lin_full)
        summed = jnp.zeros((sources.shape[0], D), jnp.float32)
        for group in range(N_TP):
            partial_value = jnp.dot(activation[:, group * half_width:(group + 1) * half_width], down_full[group * half_width:(group + 1) * half_width], preferred_element_type=jnp.float32).astype(jnp.bfloat16)
            summed = summed + lax.optimization_barrier(partial_value).astype(jnp.float32)
        return summed.astype(jnp.bfloat16)
    results = lax.map(run_expert, (slot_source.reshape(EXPERTS, device_count * CAP), gate_up, lin_up, down_weight))
    picked = results.reshape(-1, D)[slot_index].reshape(total_tokens, TOPK, D).astype(jnp.float32)
    expert_sum = lax.optimization_barrier(jnp.sum(picked * route_weights.astype(jnp.float32)[:, :, None], axis=1))
    return (mixed.astype(jnp.float32) + expert_sum).astype(jnp.bfloat16)
```

```python
import functools

import jax
import jax.numpy as jnp
from jax import lax
from jax.experimental import pallas as pl
from jax.experimental.pallas import tpu as pltpu
from jax.sharding import PartitionSpec as P

D = 2048
DK = 128
DV = 256


EPS = 1e-05
CLAMP_LIMIT = 7.0
SIGMOID_SLOPE = 1.702
TOP_PRECISION = lax.Precision.HIGHEST


COLUMN = 4
MESH = pl.DeviceIdType.MESH
VMEM = pl.BlockSpec(memory_space=pltpu.VMEM)
ANY = pl.BlockSpec(memory_space=pl.ANY)
DMA = pltpu.SemaphoreType.DMA


def push(src, dst, send, recv, sp, tp):
    return pltpu.make_async_remote_copy(
        src_ref=src,
        dst_ref=dst,
        send_sem=send,
        recv_sem=recv,
        device_id=(sp, tp),
        device_id_type=MESH,
    )


def greet(devices):
    barrier = pltpu.get_barrier_semaphore()
    for sp, tp in devices:
        pl.semaphore_signal(barrier, inc=1, device_id=(sp, tp), device_id_type=MESH)
    pl.semaphore_wait(barrier, len(devices))


def state_kernel(n, delta, decay, carried, inbox, outbox, send1, recv1, send2, recv2):
    me, core = lax.axis_index("sp"), lax.axis_index("tp")
    greet([(lax.rem(me + k, n), core) for k in range(1, n)])

    def out_copy(k):
        to = lax.rem(me + k, n)
        return push(delta.at[to], inbox.at[me], send1.at[k], recv1.at[k], to, core)

    def in_copy(k):
        frm = lax.rem(me + n - k, n)
        return push(delta.at[me], inbox.at[frm], send1.at[k], recv1.at[k], frm, core)

    def back_out(k):
        to = lax.rem(me + k, n)
        return push(outbox.at[to], carried.at[me], send2.at[k], recv2.at[k], to, core)

    def back_in(k):
        frm = lax.rem(me + n - k, n)
        return push(outbox.at[me], carried.at[frm], send2.at[k], recv2.at[k], frm, core)

    def each(act):
        lax.fori_loop(1, n, lambda k, c: (act(k), c)[1], 0)

    each(lambda k: out_copy(k).start())
    inbox[me] = delta[me]
    each(lambda k: in_copy(k).wait_recv())
    factor = decay[...]

    def step(s, total):
        outbox[s] = total.astype(jnp.bfloat16)
        return factor * total + inbox[s].astype(jnp.float32)

    lax.fori_loop(0, n, step, jnp.zeros(factor.shape, jnp.float32))
    each(lambda k: back_out(k).start())
    carried[me] = outbox[me]
    each(lambda k: back_in(k).wait_recv())
    each(lambda k: out_copy(k).wait_send())
    each(lambda k: back_out(k).wait_send())


def exchange_states(delta, decay):
    n = delta.shape[0]
    return pl.pallas_call(
        functools.partial(state_kernel, n),
        out_shape=jax.ShapeDtypeStruct(delta.shape, jnp.bfloat16),
        in_specs=[VMEM, VMEM],
        out_specs=VMEM,
        scratch_shapes=[
            pltpu.VMEM(delta.shape, jnp.bfloat16),
            pltpu.VMEM(delta.shape, jnp.bfloat16),
            DMA((n,)),
            DMA((n,)),
            DMA((n,)),
            DMA((n,)),
        ],
        compiler_params=pltpu.CompilerParams(collective_id=0, has_side_effects=True),
        name="states",
    )(delta, decay)


def partners(nz, np_):
    me, core = lax.axis_index("sp"), lax.axis_index("tp")
    z, p = me // np_, lax.rem(me, np_)
    devices = [(me, 1 - core)]
    devices += [((z ^ d) * np_ + p, core) for d in range(1, nz)]
    devices += [(z * np_ + (p ^ k), core) for k in range(1, np_)]
    return me, core, z, p, devices


def dispatch_kernel(
    nz,
    np_,
    part,
    residual,
    gain,
    picks,
    weights,
    mixed,
    landed,
    weights_in,
    part_in,
    rows,
    picks_in,
    stage,
    part_sem,
    row_send,
    row_recv,
    pick_send,
    pick_recv,
    weight_send,
    weight_recv,
    plane_send,
    plane_recv,
    core_send,
    core_recv,
    own_sem,
):
    me, core, z, p, devices = partners(nz, np_)
    other = 1 - core
    own_rows = residual.shape[0]
    cap = landed.shape[3]
    greet(devices)

    def half(which):
        return part.at[pl.ds(pl.multiple_of(which * own_rows, own_rows), own_rows)]

    swap = push(half(other), part_in, part_sem.at[0], part_sem.at[1], me, other)
    swap.start()

    def column(d, kind):
        there = z ^ d
        to = there * np_ + p
        if kind == "pick":
            return push(
                picks.at[there], picks_in.at[z], pick_send.at[d], pick_recv.at[d], to, core
            )
        if kind == "weight":
            return push(
                weights.at[there], weights_in.at[z], weight_send.at[d], weight_recv.at[d], to, core
            )
        return push(rows.at[z], rows.at[z], row_send.at[d], row_recv.at[d], to, core)

    def column_in(d, kind):
        there = z ^ d
        to = there * np_ + p
        if kind == "pick":
            return push(
                picks.at[z], picks_in.at[there], pick_send.at[d], pick_recv.at[d], to, core
            )
        if kind == "weight":
            return push(
                weights.at[z], weights_in.at[there], weight_send.at[d], weight_recv.at[d], to, core
            )
        return push(rows.at[there], rows.at[there], row_send.at[d], row_recv.at[d], to, core)

    for d in range(1, nz):
        column(d, "pick").start()
    picks_in[z] = picks[z]
    weights_in[z] = weights[z]
    swap.wait_recv()
    wide = residual[...].astype(jnp.float32) + (
        half(core)[...].astype(jnp.float32) + part_in[...].astype(jnp.float32)
    )
    mixed[...] = wide.astype(jnp.bfloat16)
    wide = mixed[...].astype(jnp.float32)
    scale = lax.rsqrt(jnp.mean(wide * wide, axis=-1, keepdims=True) + EPS)
    rows[z] = (wide * scale * gain[...]).astype(jnp.bfloat16)
    for d in range(1, nz):
        column(d, "row").start()
    for d in range(1, nz):
        column(d, "weight").start()

    def plane(d, k):
        q = p ^ k
        src = stage.at[z ^ d, pl.ds(pl.multiple_of(q * cap, cap), cap)]
        return push(
            src,
            landed.at[p, z ^ d, core],
            plane_send.at[d, k],
            plane_recv.at[d, k],
            z * np_ + q,
            core,
        )

    def plane_in(d, k):
        q = p ^ k
        src = stage.at[z ^ d, pl.ds(pl.multiple_of(q * cap, cap), cap)]
        return push(
            src,
            landed.at[q, z ^ d, core],
            plane_send.at[d, k],
            plane_recv.at[d, k],
            z * np_ + q,
            core,
        )

    def own(d):
        src = stage.at[z ^ d, pl.ds(pl.multiple_of(p * cap, cap), cap)]
        return pltpu.make_async_copy(src, landed.at[p, z ^ d, core], own_sem.at[d])

    def forward(d, k):
        where = landed.at[p ^ k, z ^ d, core]
        return push(where, where, core_send.at[d, k], core_recv.at[d, k], me, other)

    def forward_own(d):
        src = stage.at[z ^ d, pl.ds(pl.multiple_of(p * cap, cap), cap)]
        return push(
            src, landed.at[p, z ^ d, core], core_send.at[d, 0], core_recv.at[d, 0], me, other
        )

    def forward_in(d, k):
        where = landed.at[p ^ k, z ^ d, other]
        return push(where, where, core_send.at[d, k], core_recv.at[d, k], me, other)

    def each(first, act):
        lax.fori_loop(first, np_, lambda k, c: (act(k), c)[1], 0)

    width = min(512, D)
    for d in range(nz):
        if d:
            column_in(d, "pick").wait_recv()
            column_in(d, "row").wait_recv()
        there = z ^ d
        for start in range(0, D, width):
            stage[there, :, start : start + width] = jnp.dot(
                picks_in[there],
                rows[there, :, start : start + width],
                preferred_element_type=jnp.float32,
            ).astype(jnp.bfloat16)
        each(1, lambda k: plane(d, k).start())
        own(d).start()
        forward_own(d).start()
    for d in range(nz):

        def pass_on(k):
            plane_in(d, k).wait_recv()
            forward(d, k).start()

        each(1, pass_on)
    for d in range(nz):
        each(0, lambda k: forward_in(d, k).wait_recv())
        own(d).wait()
        if d:
            column_in(d, "weight").wait_recv()
    swap.wait_send()
    for d in range(nz):
        if d:
            for kind in ("pick", "row", "weight"):
                column(d, kind).wait_send()
        each(1, lambda k: plane(d, k).wait_send())
        forward_own(d).wait_send()
        each(1, lambda k: forward(d, k).wait_send())


def dispatch(part, residual, gain, picks, weights, np_, cap):
    nz = picks.shape[0]
    own_rows, width = residual.shape
    return pl.pallas_call(
        functools.partial(dispatch_kernel, nz, np_),
        out_shape=(
            jax.ShapeDtypeStruct(residual.shape, jnp.bfloat16),
            jax.ShapeDtypeStruct((np_, nz, 2, cap, width), jnp.bfloat16),
            jax.ShapeDtypeStruct(weights.shape, jnp.bfloat16),
        ),
        in_specs=[VMEM] * 5,
        out_specs=(VMEM, ANY, VMEM),
        scratch_shapes=[
            pltpu.VMEM(residual.shape, jnp.bfloat16),
            pltpu.VMEM((nz, own_rows, width), jnp.bfloat16),
            pltpu.VMEM(picks.shape, jnp.bfloat16),
            pltpu.VMEM((nz, np_ * cap, width), jnp.bfloat16),
            DMA((2,)),
            DMA((nz,)),
            DMA((nz,)),
            DMA((nz,)),
            DMA((nz,)),
            DMA((nz,)),
            DMA((nz,)),
            DMA((nz, np_)),
            DMA((nz, np_)),
            DMA((nz, np_)),
            DMA((nz, np_)),
            DMA((nz,)),
        ],
        compiler_params=pltpu.CompilerParams(collective_id=1, has_side_effects=True),
        name="dispatch",
    )(part, residual, gain, picks, weights)


def combine_kernel(
    nz,
    np_,
    halves,
    weights,
    mixed,
    result,
    own_half,
    other_half,
    stage,
    back,
    sums,
    final,
    own_sem,
    core_send,
    core_recv,
    plane_send,
    plane_recv,
    col_send,
    col_recv,
):
    me, core, z, p, devices = partners(nz, np_)
    other = 1 - core
    cap = halves.shape[3]

    def load(d, k):
        return pltpu.make_async_copy(
            halves.at[p ^ k, z ^ d, core], own_half.at[p ^ k, z ^ d], own_sem.at[d, k]
        )

    def across(d, k):
        return push(
            halves.at[p ^ k, z ^ d, other],
            other_half.at[p ^ k, z ^ d],
            core_send.at[d, k],
            core_recv.at[d, k],
            me,
            other,
        )

    def slot(which):
        return pl.ds(pl.multiple_of(which * cap, cap), cap)

    def plane(d, k):
        q = p ^ k
        return push(
            stage.at[q, z ^ d],
            back.at[z ^ d, slot(p)],
            plane_send.at[d, k],
            plane_recv.at[d, k],
            z * np_ + q,
            core,
        )

    def plane_in(d, k):
        q = p ^ k
        return push(
            stage.at[q, z ^ d],
            back.at[z ^ d, slot(q)],
            plane_send.at[d, k],
            plane_recv.at[d, k],
            z * np_ + q,
            core,
        )

    def column(d):
        return push(
            sums.at[z ^ d],
            final.at[z],
            col_send.at[d],
            col_recv.at[d],
            (z ^ d) * np_ + p,
            core,
        )

    def column_in(d):
        return push(
            sums.at[z],
            final.at[z ^ d],
            col_send.at[d],
            col_recv.at[d],
            (z ^ d) * np_ + p,
            core,
        )

    def each(first, act):
        lax.fori_loop(first, np_, lambda k, c: (act(k), c)[1], 0)

    order = list(range(nz - 1, -1, -1))
    for d in order:
        each(0, lambda k: load(d, k).start())
    greet(devices)
    for d in order:
        each(0, lambda k: across(d, k).start())
    for d in order:

        def joined(k):
            load(d, k).wait()
            across(d, k).wait_recv()
            there = (p ^ k, z ^ d)
            return (
                own_half[there].astype(jnp.float32) + other_half[there].astype(jnp.float32)
            ).astype(jnp.bfloat16)

        def send_on(k):
            stage[p ^ k, z ^ d] = joined(k)
            plane(d, k).start()

        each(1, send_on)
        back[z ^ d, slot(p)] = joined(0)
    width = min(512, D)
    for d in order:
        each(1, lambda k: plane_in(d, k).wait_recv())
        there = z ^ d
        if d:
            for start in range(0, D, width):
                sums[there, :, start : start + width] = jnp.dot(
                    weights[there],
                    back[there, :, start : start + width],
                    preferred_element_type=jnp.float32,
                ).astype(jnp.bfloat16)
            column(d).start()
    for d in range(1, nz):
        column_in(d).wait_recv()
    for start in range(0, D, width):
        cols = slice(start, start + width)
        total = jnp.dot(weights[z], back[z, :, cols], preferred_element_type=jnp.float32)
        for d in range(1, nz):
            total = total + final[z ^ d, :, cols].astype(jnp.float32)
        result[:, cols] = (mixed[:, cols].astype(jnp.float32) + total).astype(jnp.bfloat16)
    for d in order:
        each(0, lambda k: across(d, k).wait_send())
        each(1, lambda k: plane(d, k).wait_send())
        if d:
            column(d).wait_send()


def combine(halves, weights, mixed):
    np_, nz, _, cap, width = halves.shape
    own_rows = mixed.shape[0]
    return pl.pallas_call(
        functools.partial(combine_kernel, nz, np_),
        out_shape=jax.ShapeDtypeStruct(mixed.shape, jnp.bfloat16),
        in_specs=[ANY, VMEM, VMEM],
        out_specs=VMEM,
        scratch_shapes=[
            pltpu.VMEM((np_, nz, cap, width), jnp.bfloat16),
            pltpu.VMEM((np_, nz, cap, width), jnp.bfloat16),
            pltpu.VMEM((np_, nz, cap, width), jnp.bfloat16),
            pltpu.VMEM((nz, np_ * cap, width), jnp.bfloat16),
            pltpu.VMEM((nz, own_rows, width), jnp.bfloat16),
            pltpu.VMEM((nz, own_rows, width), jnp.bfloat16),
            DMA((nz, np_)),
            DMA((nz, np_)),
            DMA((nz, np_)),
            DMA((nz, np_)),
            DMA((nz, np_)),
            DMA((nz,)),
            DMA((nz,)),
        ],
        compiler_params=pltpu.CompilerParams(collective_id=2, has_side_effects=True),
        name="combine",
    )(halves, weights, mixed)


def expert_act(row_block, gate_part, lin_part):
    gate_pre = jnp.dot(row_block, gate_part, preferred_element_type=jnp.float32)
    lin_pre = jnp.dot(row_block, lin_part, preferred_element_type=jnp.float32)
    gate_clip = jnp.minimum(gate_pre, CLAMP_LIMIT)
    lin_clip = jnp.clip(lin_pre, -CLAMP_LIMIT, CLAMP_LIMIT)
    return (gate_clip * jax.nn.sigmoid(SIGMOID_SLOPE * gate_clip) * (lin_clip + 1.0)).astype(
        jnp.bfloat16
    )


def local(
    queries,
    keys,
    values,
    out_gate,
    decay_rate,
    residual,
    out_weight,
    ffn_gain,
    route_ids,
    route_weights,
    gate_up,
    lin_up,
    down_weight,
):
    block_len = queries.shape[0]
    local_heads = decay_rate.shape[0]
    log_gamma = -decay_rate
    query_heads = queries.astype(jnp.float32).reshape(block_len, local_heads, DK).transpose(1, 0, 2)
    per_head_keys = keys.astype(jnp.float32).reshape(block_len, local_heads, DK).transpose(
        1, 0, 2
    ) * DK ** (-0.5)
    per_head_values = (
        values.astype(jnp.float32).reshape(block_len, local_heads, DV).transpose(1, 0, 2)
    )
    positions = jnp.arange(block_len, dtype=jnp.float32)
    offsets = positions[:, None] - positions[None, :]
    causal = offsets >= 0
    decay_mask = jnp.where(
        causal[None], jnp.exp(jnp.where(causal, offsets, 0.0)[None] * log_gamma[:, None, None]), 0.0
    )
    trailing_decay = jnp.exp((block_len - 1.0 - positions)[None, :] * log_gamma[:, None])
    lead_decay = jnp.exp((positions + 1.0)[None, :] * log_gamma[:, None])
    chain_decay = jnp.exp(block_len * log_gamma)
    attention_scores = (
        jnp.einsum("hqd,hkd->hqk", query_heads, per_head_keys, precision=TOP_PRECISION) * decay_mask
    )
    intra_block_term = jnp.einsum(
        "zfp,zpn->zfn", attention_scores, per_head_values, precision=TOP_PRECISION
    )
    state_delta = jnp.einsum(
        "mxs,mxq->msq",
        per_head_keys * trailing_decay[:, :, None],
        per_head_values,
        precision=TOP_PRECISION,
    )
    peers = lax.axis_size("sp")
    state_rows = local_heads * DK // peers
    head_of_row = (lax.axis_index("sp") * state_rows + jnp.arange(state_rows)) // DK
    row_decay = jnp.sum(
        jnp.where(head_of_row[:, None] == jnp.arange(local_heads)[None], chain_decay[None], 0.0),
        axis=1,
    )
    carried = (
        exchange_states(
            state_delta.astype(jnp.bfloat16).reshape(peers, state_rows, DV),
            jnp.broadcast_to(row_decay[:, None], (state_rows, DV)),
        )
        .reshape(local_heads, DK, DV)
        .astype(jnp.float32)
    )
    cross_term = (
        jnp.einsum("hqd,hdv->hqv", query_heads, carried, precision=TOP_PRECISION)
        * lead_decay[:, :, None]
    )
    retained = intra_block_term + cross_term
    normed = retained * lax.rsqrt(jnp.mean(retained * retained, axis=-1, keepdims=True) + EPS)
    gated = (
        normed.transpose(1, 0, 2).reshape(block_len, local_heads * DV)
        * jax.nn.silu(out_gate.astype(jnp.float32))
    ).astype(jnp.bfloat16)
    part = jnp.dot(gated, out_weight, preferred_element_type=jnp.float32).astype(jnp.bfloat16)
    own_rows, top_count = route_ids.shape
    capacity = own_rows * top_count * lax.axis_size("tp") // peers
    column = min(COLUMN, peers)
    plane = peers // column
    hits = route_ids[:, :, None] == jnp.arange(peers, dtype=jnp.int32)[None, None, :]
    named = jnp.any(hits, axis=1)
    weight_of = jnp.sum(jnp.where(hits, route_weights[:, :, None], 0.0), axis=1)
    earlier = jnp.arange(own_rows)[:, None] > jnp.arange(own_rows)[None, :]
    rank = jnp.dot(
        earlier.astype(jnp.bfloat16),
        named.astype(jnp.bfloat16),
        preferred_element_type=jnp.float32,
    ).astype(jnp.int32)
    slot_of = jnp.where(named, rank, -1)
    slots = jnp.arange(capacity, dtype=jnp.int32)
    picks = (slot_of.T[:, None, :] == slots[None, :, None]).astype(jnp.bfloat16)
    picks = picks.reshape(column, plane * capacity, own_rows)
    weights = jnp.where(
        slot_of.reshape(own_rows, column, plane).transpose(1, 0, 2)[:, :, :, None] == slots,
        weight_of.reshape(own_rows, column, plane).transpose(1, 0, 2)[:, :, :, None],
        0.0,
    ).astype(jnp.bfloat16)
    weights = weights.reshape(column, own_rows, plane * capacity)
    mixed, landed, weights_in = dispatch(
        part, residual, ffn_gain[None, :], picks, weights, plane, capacity
    )
    activation = expert_act(landed.reshape(-1, D), gate_up[0], lin_up[0])
    halves = (
        jnp.dot(activation, down_weight[0], preferred_element_type=jnp.float32)
        .astype(jnp.bfloat16)
        .reshape(landed.shape)
    )
    return combine(halves, weights_in, mixed)


def solution(mesh):
    placed = (
        P("sp", "tp"),
        P("sp", "tp"),
        P("sp", "tp"),
        P("sp", "tp"),
        P("tp"),
        P(("sp", "tp"), None),
        P("tp", None),
        P(),
        P(("sp", "tp"), None),
        P(("sp", "tp"), None),
        P("sp", None, "tp"),
        P("sp", None, "tp"),
        P("sp", "tp", None),
    )
    return jax.shard_map(
        local, mesh=mesh, in_specs=placed, out_specs=P(("sp", "tp"), None), check_vma=False
    )
```
